32 devices in a mesh: ep: 4 (over y, x), tp: 8 (over z, core).
Axes of the slice: x: 2, y: 2, z: 4, core: 2. Of those that a mesh axis runs over, the one named last changes fastest.
Arguments:
- tokens: bfloat16 [128, 4096], P('ep'), may hold values from -6 to 6
- state_matrix: float32 [128, 16, 128, 128], P('ep', 'tp'), may hold values from -1.5 to 1.5
- state_norm: float32 [128, 16, 128], P('ep', 'tp'), may hold values from -4 to 4
- state_max: float32 [128, 16], P('ep', 'tp'), may hold values from -5 to 5
- mixer_gain: float32 [4096], replicated, may hold values from 0.1 to 1.9
- w_query: bfloat16 [4096, 2048], P('ep', 'tp'), may hold values from -0.09375 to 0.09375
- w_key: bfloat16 [4096, 2048], P('ep', 'tp'), may hold values from -0.09375 to 0.09375
- w_value: bfloat16 [4096, 2048], P('ep', 'tp'), may hold values from -0.09375 to 0.09375
- w_outgate: bfloat16 [4096, 2048], P('ep', 'tp'), may hold values from -0.09375 to 0.09375
- w_ingate: bfloat16 [4096, 16], replicated, may hold values from -0.09375 to 0.09375
- w_forget: bfloat16 [4096, 16], replicated, may hold values from -0.09375 to 0.09375
- forget_bias: float32 [16], replicated, may hold values from -2 to 4
- w_proj: bfloat16 [2048, 4096], P('tp', 'ep'), may hold values from -0.125 to 0.125
- ffn_gain: float32 [4096], replicated, may hold values from 0.1 to 1.9
- w_branch: bfloat16 [4096], replicated, may hold values from -0.09375 to 0.09375
- routes: int32 [128, 2], P('ep'), may hold values from 0 to 3, all different within a row; in each aligned block of 32 rows (0 to 31, 32 to 63, ...) at most 22 rows name the same one
- route_weight: float32 [128, 2], P('ep'), may hold values from 0.2 to 1
- expert_gate: bfloat16 [4, 4096, 4096], P('ep', None, 'tp'), may hold values from -0.09375 to 0.09375
- expert_up: bfloat16 [4, 4096, 4096], P('ep', None, 'tp'), may hold values from -0.09375 to 0.09375
- expert_down: bfloat16 [4, 4096, 4096], P('ep', 'tp'), may hold values from -0.09375 to 0.09375
- dense_gate: bfloat16 [4096, 8192], P('ep', 'tp'), may hold values from -0.09375 to 0.09375
- dense_up: bfloat16 [4096, 8192], P('ep', 'tp'), may hold values from -0.09375 to 0.09375
- dense_down: bfloat16 [8192, 4096], P('tp', 'ep'), may hold values from -0.0625 to 0.0625
Outputs:
- layer_out: bfloat16 [128, 4096], P('ep')
- new_matrix: float32 [128, 16, 128, 128], P('ep', 'tp')
- new_norm: float32 [128, 16, 128], P('ep', 'tp')
- new_max: float32 [128, 16], P('ep', 'tp')
The draws below stay inside these ranges and needn't reach their ends.
Inputs may be any that keep to these rules, and one draw needn't show every extreme that they name: `routes`: each row names 2 different experts. Among the rows of one index of ep (32 sequences) no expert is named more than 22 times, and in some such group one expert is named exactly 22 times.
All inputs are finite; a program needn't handle non-finite values.
Results may differ from the reference program's by a relative error of at most 0.012.
Values may be sent and summed in bfloat16 or wider, within the bound.
A program may use at most 64 MiB of HBM per device.

```python
import math
import jax
import jax.numpy as jnp
import numpy as np
from jax import lax

D = 4096
HEADS = 16
HDIM = 128
MW = 2048
FFD = 8192
FFE = 4096
TOPK = 2
SEQS = 32
BATCH = 128
EXPERTS = 4
CAP = 22
N_EP = 4


def shard_levels(stream_key, shape, pieces, low, high):
    def one(axis_at, parts):
        draws = jax.random.uniform(jax.random.fold_in(jax.random.fold_in(stream_key, 6), axis_at), (parts,), jnp.float32, low / len(pieces), high / len(pieces))
        return jnp.repeat(jnp.exp(draws), shape[axis_at] // parts).reshape((-1,) + (1,) * (len(shape) - axis_at - 1))

    level = one(*pieces[0])
    for cut in pieces[1:]:
        level = level * one(*cut)
    return level


def shared_out(key, own, number, rows, amount, top, limit, slope):
    ranking = jax.random.permutation(key, amount)
    crowded, usual = load_shares(amount, rows * top, limit, slope, True), load_shares(amount, rows * top, limit, slope, False)
    places = jnp.arange(amount)

    def named(lengths, turn):
        used = int((lengths > 0).sum())
        fixed = max(1, used // 4)
        shifted = fixed + (places - fixed + turn * (used - fixed)) % max(1, amount - fixed)
        return jnp.zeros((amount,), jnp.int32).at[ranking[jnp.where(places < fixed, places, shifted)]].set(jnp.asarray(lengths, jnp.int32))

    lengths = jnp.where(number % 4 == 0, named(crowded, number // 4), named(usual, number - number // 4 - 1))
    mixed = jax.random.permutation(jax.random.fold_in(own, 3), amount)
    giver, receiver = mixed[0:amount // 2 * 2:2], mixed[1:amount // 2 * 2:2]
    slack = jnp.minimum(lengths[giver] - 1, limit - lengths[receiver]) // 2
    slack = jnp.where((giver == ranking[0]) | (receiver == ranking[0]) | (lengths[receiver] == 0), 0, jnp.maximum(slack, 0))
    shifted = jax.random.randint(jax.random.fold_in(own, 4), (amount // 2,), 0, 1 << 20) % (slack + 1)
    lengths = lengths.at[giver].add(-shifted).at[receiver].add(shifted)
    members = jnp.searchsorted(jnp.cumsum(lengths), jnp.arange(rows * top), side="right").astype(jnp.int32)
    grid = members.reshape(top, rows).T
    grid = grid[jax.random.permutation(jax.random.fold_in(own, 1), rows)]
    turn = jax.random.randint(jax.random.fold_in(own, 2), (rows, 1), 0, top)
    return jnp.take_along_axis(grid, (jnp.arange(top)[None, :] + turn) % top, axis=1)


def load_shares(number_of, total, limit, lean, full):
    portions = [(1 << 20) // math.isqrt(standing ** lean) + 1 for standing in range(1, number_of + 1)]
    largest = limit if full else min(limit, max(-(-total // number_of), total * portions[0] // sum(portions)))
    least = 1 if total - largest >= number_of - 1 else 0
    given, surplus = [largest] + [least] * (number_of - 1), total - largest - least * (number_of - 1)
    while surplus > 0:
        movable = [i for i in range(1, number_of) if given[i] < largest] or [i for i in range(1, number_of) if given[i] < limit]
        pool, left = sum([portions[i] for i in movable]), surplus
        for i in movable:
            addition = min(limit - given[i], max(1, left * portions[i] // pool), surplus)
            given[i] = given[i] + addition
            surplus = surplus - addition
    return np.array(given)


def bell_draw(stream_key, extent, spread, reach, pieces=(), held_as=jnp.bfloat16):
    result = spread * jax.random.normal(stream_key, extent, jnp.float32)
    if pieces:
        result = result * shard_levels(stream_key, extent, pieces, -0.22, 0.18)
    return jnp.clip(result, -reach, reach).astype(held_as)


def setup_inputs(seed: int = 0) -> dict:
    key_of = jax.random.split(jax.random.key(seed), 24)
    tokens = bell_draw(key_of[0], (BATCH, D), 1.0, 6.0, ((0, 4),))
    state_matrix = bell_draw(key_of[1], (BATCH, HEADS, HDIM, HDIM), 0.1, 1.5, ((0, 4), (1, 8)), jnp.float32)
    state_norm = bell_draw(key_of[2], (BATCH, HEADS, HDIM), 0.3, 4.0, ((0, 4), (1, 8)), jnp.float32)
    state_max = bell_draw(key_of[3], (BATCH, HEADS), 1.0, 5.0, ((0, 4), (1, 8)), jnp.float32)
    mixer_gain = jnp.clip(1.0 + 0.18 * jax.random.normal(key_of[4], (D,), jnp.float32), 0.1, 1.9)
    w_query = bell_draw(key_of[5], (D, MW), D ** -0.5, 0.09375, ((0, 4), (1, 8)))
    w_key = bell_draw(key_of[6], (D, MW), D ** -0.5, 0.09375, ((0, 4), (1, 8)))
    w_value = bell_draw(key_of[7], (D, MW), D ** -0.5, 0.09375, ((0, 4), (1, 8)))
    w_outgate = bell_draw(key_of[8], (D, MW), D ** -0.5, 0.09375, ((0, 4), (1, 8)))
    w_ingate = bell_draw(key_of[9], (D, HEADS), D ** -0.5, 0.09375)
    w_forget = bell_draw(key_of[10], (D, HEADS), D ** -0.5, 0.09375)
    forget_bias = jnp.clip(jax.random.uniform(key_of[11], (HEADS,), jnp.float32, -2.0, 4.0), -2.0, 4.0)
    w_proj = bell_draw(key_of[12], (MW, D), MW ** -0.5, 0.125, ((0, 8), (1, 4)))
    ffn_gain = jnp.clip(1.0 + 0.18 * jax.random.normal(key_of[13], (D,), jnp.float32), 0.1, 1.9)
    w_branch = bell_draw(key_of[14], (D,), D ** -0.5, 0.09375)
    routes_keys = jax.random.split(jax.random.fold_in(key_of[15], 1), BATCH // SEQS)
    routes_turns = jax.random.permutation(jax.random.fold_in(key_of[15], 3), BATCH // SEQS)
    routes = jax.vmap(lambda own, number: shared_out(jax.random.fold_in(key_of[15], 2), own, number, SEQS, EXPERTS, TOPK, CAP, 2))(routes_keys, routes_turns).reshape((BATCH, TOPK))
    route_weight = jnp.clip(jnp.exp(math.log(1.0) - 1.609438 * jax.random.uniform(key_of[16], (BATCH, TOPK), jnp.float32) ** shard_levels(key_of[16], (BATCH, TOPK), ((0, 4),), -0.2, 0.2)), 0.2, 1.0)
    expert_gate = bell_draw(key_of[17], (EXPERTS, D, FFE), D ** -0.5, 0.09375, ((0, 4), (2, 8)))
    expert_up = bell_draw(key_of[18], (EXPERTS, D, FFE), D ** -0.5, 0.09375, ((0, 4), (2, 8)))
    expert_down = bell_draw(key_of[19], (EXPERTS, FFE, D), FFE ** -0.5, 0.09375, ((0, 4), (1, 8)))
    dense_gate = bell_draw(key_of[20], (D, FFD), D ** -0.5, 0.09375, ((0, 4), (1, 8)))
    dense_up = bell_draw(key_of[21], (D, FFD), D ** -0.5, 0.09375, ((0, 4), (1, 8)))
    dense_down = bell_draw(key_of[22], (FFD, D), FFD ** -0.5, 0.0625, ((0, 8), (1, 4)))
    return dict(tokens=tokens, state_matrix=state_matrix, state_norm=state_norm, state_max=state_max, mixer_gain=mixer_gain, w_query=w_query, w_key=w_key, w_value=w_value, w_outgate=w_outgate, w_ingate=w_ingate, w_forget=w_forget, forget_bias=forget_bias, w_proj=w_proj, ffn_gain=ffn_gain, w_branch=w_branch, routes=routes, route_weight=route_weight, expert_gate=expert_gate, expert_up=expert_up, expert_down=expert_down, dense_gate=dense_gate, dense_up=dense_up, dense_down=dense_down)


EPS = 1e-06

def rms_scale(values, gain):
    wide = values.astype(jnp.float32)
    return wide * lax.rsqrt(lax.optimization_barrier(jnp.mean(wide * wide, axis=-1, keepdims=True)) + EPS) * gain.astype(jnp.float32)

def slot_numbers(flat_routes, experts_all):
    onehot = (flat_routes[:, None] == jnp.arange(experts_all, dtype=jnp.int32)[None, :]).astype(jnp.int32)
    before = jnp.cumsum(onehot, axis=0) - onehot
    return lax.optimization_barrier(jnp.sum(before * onehot, axis=1)).astype(jnp.int32)

def memory_step(query_all, key_all, value_all, outgate, gate_in, gate_forget, state_matrix, state_norm, state_max):
    row_count, head_count = gate_in.shape
    head_size = state_matrix.shape[-1]
    heads_q = query_all.reshape(row_count, head_count, head_size)
    heads_k = key_all.reshape(row_count, head_count, head_size) * head_size ** (-0.5)
    heads_v = value_all.reshape(row_count, head_count, head_size)
    log_keep = jax.nn.log_sigmoid(gate_forget)
    new_max = jnp.maximum(log_keep + state_max, gate_in)
    keep_factor = jnp.exp(log_keep + state_max - new_max)
    write_factor = jnp.exp(gate_in - new_max)
    new_matrix = keep_factor[:, :, None, None] * state_matrix + write_factor[:, :, None, None] * heads_k[:, :, :, None] * heads_v[:, :, None, :]
    new_norm = keep_factor[:, :, None] * state_norm + write_factor[:, :, None] * heads_k
    numer = jnp.einsum('bhk,bhkv->bhv', heads_q, new_matrix, precision=lax.Precision.HIGHEST)
    denom = lax.optimization_barrier(jnp.sum(heads_q * new_norm, axis=-1))
    cell = numer / jnp.maximum(jnp.abs(denom), 1.0)[:, :, None]
    gated = jax.nn.sigmoid(outgate.reshape(row_count, head_count, head_size)) * cell
    mixed_heads = gated.reshape(row_count, head_count * head_size).astype(jnp.bfloat16)
    return (mixed_heads, new_matrix, new_norm, new_max)

def reference(tokens, state_matrix, state_norm, state_max, mixer_gain, w_query, w_key, w_value, w_outgate, w_ingate, w_forget, forget_bias, w_proj, ffn_gain, w_branch, routes, route_weight, expert_gate, expert_up, expert_down, dense_gate, dense_up, dense_down):
    normed = rms_scale(tokens, mixer_gain).astype(jnp.bfloat16)
    query_all = jnp.dot(normed, w_query, preferred_element_type=jnp.float32)
    key_all = jnp.dot(normed, w_key, preferred_element_type=jnp.float32)
    value_all = jnp.dot(normed, w_value, preferred_element_type=jnp.float32)
    outgate = jnp.dot(normed, w_outgate, preferred_element_type=jnp.float32)
    gate_in = jnp.dot(normed, w_ingate, preferred_element_type=jnp.float32)
    gate_forget = jnp.dot(normed, w_forget, preferred_element_type=jnp.float32) + forget_bias
    mixed_heads, new_matrix, new_norm, new_max = memory_step(query_all, key_all, value_all, outgate, gate_in, gate_forget, state_matrix, state_norm, state_max)
    mixer_out = jnp.dot(mixed_heads, w_proj, preferred_element_type=jnp.float32)
    residual = (tokens.astype(jnp.float32) + mixer_out).astype(jnp.bfloat16)
    ffn_in = rms_scale(residual, ffn_gain).astype(jnp.bfloat16)
    branch_share = jax.nn.sigmoid(jnp.dot(ffn_in, w_branch, preferred_element_type=jnp.float32))
    dense_hidden = (jax.nn.silu(jnp.dot(ffn_in, dense_gate, preferred_element_type=jnp.float32)) * jnp.dot(ffn_in, dense_up, preferred_element_type=jnp.float32)).astype(jnp.bfloat16)
    dense_out = jnp.dot(dense_hidden, dense_down, preferred_element_type=jnp.float32)
    group_routes = routes.reshape(N_EP, SEQS * TOPK)
    slots = jax.vmap(lambda group_row: slot_numbers(group_row, EXPERTS))(group_routes)
    group_ids = jnp.broadcast_to(jnp.arange(N_EP, dtype=jnp.int32)[:, None], group_routes.shape)
    repeated = jnp.repeat(ffn_in, TOPK, axis=0).reshape(N_EP, SEQS * TOPK, D)
    buffers = jnp.zeros((EXPERTS, N_EP, CAP, D), jnp.bfloat16).at[group_routes, group_ids, slots].set(repeated)

    def one_expert(index):
        rows_in = buffers[index].reshape(N_EP * CAP, D)
        hidden = (jax.nn.silu(jnp.dot(rows_in, expert_gate[index], preferred_element_type=jnp.float32)) * jnp.dot(rows_in, expert_up[index], preferred_element_type=jnp.float32)).astype(jnp.bfloat16)
        return jnp.dot(hidden, expert_down[index], preferred_element_type=jnp.float32).reshape(N_EP, CAP, D)
    results = lax.map(one_expert, jnp.arange(EXPERTS, dtype=jnp.int32))
    picked = results[group_routes, group_ids, slots].reshape(N_EP * SEQS, TOPK, D)
    shares = route_weight / lax.optimization_barrier(jnp.sum(route_weight, axis=1, keepdims=True))
    expert_rows = lax.optimization_barrier(jnp.sum(shares[:, :, None] * picked, axis=1))
    total_ffn = expert_rows + branch_share[:, None] * dense_out
    layer_out = (residual.astype(jnp.float32) + total_ffn).astype(jnp.bfloat16)
    return (layer_out, new_matrix, new_norm, new_max)
```

```python
import functools

import jax
import jax.numpy as jnp
from jax import lax
from jax.experimental import pallas as pl
from jax.experimental.pallas import tpu as pltpu
from jax.sharding import PartitionSpec as P

EPS = 1e-06
F32 = jnp.float32
BF16 = jnp.bfloat16
MESH = pl.DeviceIdType.MESH


def remote(src, dst, sems, phase, k, peer):
    return pltpu.make_async_remote_copy(
        src_ref=src,
        dst_ref=dst,
        send_sem=sems[0].at[phase, k],
        recv_sem=sems[1].at[phase, k],
        device_id=peer,
        device_id_type=MESH,
    )


def around(n, me, make):
    copies = [make(k, lax.rem(me + k, n)) for k in range(1, n)]
    for copy in copies:
        copy.start()
    return copies


def finish(copies):
    for copy in copies:
        copy.wait()


def project_kernel(
    n_ep, n_tp,
    tokens, gain, w_q, w_k, w_v, w_o, w_in, w_fg, bias,
    proj, gates, spread,
    arrived, weights, gate_w, outgoing, incoming, send_sem, recv_sem, load_sem,
):
    e, t = lax.axis_index("ep"), lax.axis_index("tp")
    seqs, width = tokens.shape
    block = width // n_ep
    cols = w_q.shape[1]
    heads_all = bias.shape[1]
    heads = heads_all // n_tp
    sems = (send_sem, recv_sem)
    barrier = pltpu.get_barrier_semaphore()
    for k in range(1, n_ep):
        pl.semaphore_signal(
            barrier, inc=1, device_id={"ep": lax.rem(e + k, n_ep)}, device_id_type=MESH
        )
    loads = [
        pltpu.make_async_copy(src, dst, load_sem.at[i])
        for i, (src, dst) in enumerate(
            [(w_in, gate_w.at[0]), (w_fg, gate_w.at[1])]
            + [(w, weights.at[j]) for j, w in enumerate((w_q, w_k, w_v, w_o))]
        )
    ]
    for load in loads:
        load.start()
    pl.semaphore_wait(barrier, n_ep - 1)

    def columns(index):
        return pl.ds(pl.multiple_of(index * block, block), block)

    copies = around(
        n_ep, e,
        lambda k, p: remote(tokens.at[:, columns(p)], arrived.at[e], sems, 0, k, {"ep": p}),
    )
    wide = tokens[...].astype(F32)
    scale = lax.rsqrt(jnp.mean(wide * wide, axis=1, keepdims=True) + EPS)
    normed = (wide * scale * gain[...]).astype(BF16)
    loads[0].wait()
    loads[1].wait()
    gate_in = jnp.dot(normed, gate_w[0], preferred_element_type=F32)
    gate_fg = jnp.dot(normed, gate_w[1], preferred_element_type=F32) + bias[...]
    lane = lax.broadcasted_iota(jnp.int32, gate_in.shape, 1)
    for h in range(heads):
        mine = lane == t * heads + h
        gates[:, h : h + 1] = jnp.sum(jnp.where(mine, gate_in, 0.0), axis=1, keepdims=True)
        gates[:, heads + h : heads + h + 1] = jnp.sum(
            jnp.where(mine, gate_fg, 0.0), axis=1, keepdims=True
        )
    spread[e] = tokens[:, columns(e)]
    finish(copies)
    for k in range(1, n_ep):
        p = lax.rem(e + k, n_ep)
        spread[p] = arrived[p]
    scaled = spread[...].astype(F32).reshape(n_ep * seqs, block) * gain[:, columns(e)]
    scaled = scaled.astype(BF16)
    for j in range(4):
        loads[2 + j].wait()
        part = jnp.dot(scaled, weights[j], preferred_element_type=F32)
        outgoing[:, :, j * cols : (j + 1) * cols] = part.reshape(n_ep, seqs, cols).astype(BF16)
    finish(
        around(
            n_ep, e,
            lambda k, p: remote(outgoing.at[p], incoming.at[e], sems, 1, k, {"ep": p}),
        )
    )
    total = outgoing[e].astype(F32)
    for k in range(1, n_ep):
        total = total + incoming[lax.rem(e + k, n_ep)].astype(F32)
    proj[...] = total * scale


def cell_kernel(proj, gates, matrix, norm, top, mixed, new_matrix, new_norm, new_top):
    rows, heads, size, _ = matrix.shape
    gate_in = gates[:, :heads]
    gate_fg = gates[:, heads:]
    log_keep = jnp.minimum(gate_fg, 0.0) - jnp.log1p(jnp.exp(-jnp.abs(gate_fg)))
    highest = jnp.maximum(log_keep + top[...], gate_in)
    new_top[...] = highest
    keep = jnp.exp(log_keep + top[...] - highest)
    write = jnp.exp(gate_in - highest)
    width = heads * size
    for h in range(heads):
        at = h * size
        q = proj[:, at : at + size]
        key = proj[:, width + at : width + at + size] * (size ** (-0.5))
        val = proj[:, 2 * width + at : 2 * width + at + size]
        gate = proj[:, 3 * width + at : 3 * width + at + size]
        keep_h = keep[:, h : h + 1]
        added = write[:, h : h + 1] * key
        normal = keep_h * norm[:, h, :] + added
        new_norm[:, h, :] = normal
        denom = jnp.maximum(jnp.abs(jnp.sum(q * normal, axis=1, keepdims=True)), 1.0)
        q_t = q.T
        added_t = added.T
        numer = []
        for b in range(rows):
            fresh = keep_h[b : b + 1] * matrix[b, h] + added_t[:, b : b + 1] * val[b : b + 1]
            new_matrix[b, h] = fresh
            numer.append(jnp.sum(q_t[:, b : b + 1] * fresh, axis=0, keepdims=True))
        cell = jnp.concatenate(numer, axis=0) / denom
        mixed[:, at : at + size] = cell / (1.0 + jnp.exp(-gate))


def sigmoid(x):
    return 1.0 / (1.0 + jnp.exp(-x))


def ffn_kernel(
    n_ep, n_tp,
    mixed, spread, gain, branch, routes, route_weight,
    w_proj, d_gate, d_up, e_gate, e_up, d_down, e_down,
    out,
    v_proj, v_dgate, v_dup, v_egate, v_eup, v_ddown, v_edown,
    heads_all, shares, part, part_in, full, dense_part, dense_in, dense_hid,
    scale_ref, dense_out, halves, half_in, summed, summed_in, strips, strips_in, pieces,
    send_sem, recv_sem, load_sem,
):
    e, t = lax.axis_index("ep"), lax.axis_index("tp")
    core = lax.rem(t, 2)
    z = lax.div(t, 2)
    n_z = n_tp // 2
    seqs = mixed.shape[0]
    rows = n_ep * seqs
    chunk, block = spread.shape[1], spread.shape[2]
    width = n_ep * block
    hidden = d_gate.shape[1]
    local = e_gate.shape[0]
    sems = (send_sem, recv_sem)
    sibling = {"tp": t + 1 - 2 * core}
    half_t = n_tp // 2
    strip = width // n_tp

    barrier = pltpu.get_barrier_semaphore()
    for k in range(1, n_ep):
        pl.semaphore_signal(
            barrier, inc=1, device_id={"ep": lax.rem(e + k, n_ep)}, device_id_type=MESH
        )
    for k in range(1, n_tp):
        pl.semaphore_signal(
            barrier, inc=1, device_id={"tp": lax.rem(t + k, n_tp)}, device_id_type=MESH
        )
    loads = [
        pltpu.make_async_copy(src, dst, load_sem.at[i])
        for i, (src, dst) in enumerate(
            [(w_proj, v_proj), (d_gate, v_dgate), (d_up, v_dup), (e_gate, v_egate),
             (e_up, v_eup), (d_down, v_ddown), (e_down, v_edown)]
        )
    ]
    for load in loads:
        load.start()

    heads_all[e] = mixed[...].astype(BF16)
    weight = route_weight[...]
    share = weight / jnp.sum(weight, axis=1, keepdims=True)
    lane = lax.broadcasted_iota(jnp.int32, (seqs, shares.shape[2]), 1)
    table = jnp.zeros((seqs, shares.shape[2]), F32)
    for k in range(routes.shape[1]):
        table = table + jnp.where(lane == routes[:, k : k + 1], share[:, k : k + 1], 0.0)
    shares[e] = table
    pl.semaphore_wait(barrier, n_ep + n_tp - 2)

    copies = around(
        n_ep, e,
        lambda k, p: remote(heads_all.at[e], heads_all.at[e], sems, 0, k, {"ep": p}),
    )
    share_copies = around(
        n_ep, e, lambda k, p: remote(shares.at[e], shares.at[e], sems, 1, k, {"ep": p})
    )
    loads[0].wait()
    finish(copies)
    cols = heads_all.shape[2]
    mixer = jnp.dot(
        heads_all[...].reshape(rows, cols), v_proj[...], preferred_element_type=F32
    )
    part[...] = mixer.reshape(n_tp, chunk, block).astype(BF16)
    finish(
        around(
            n_tp, t, lambda k, p: remote(part.at[p], part_in.at[t], sems, 2, k, {"tp": p})
        )
    )
    total = part[t].astype(F32)
    for k in range(1, n_tp):
        total = total + part_in[lax.rem(t + k, n_tp)].astype(F32)
    full[e, t] = (spread[t].astype(F32) + total).astype(BF16)
    finish(
        around(
            n_tp, t,
            lambda k, p: remote(full.at[e, t], full.at[e, t], sems, 3, k, {"tp": p}),
        )
    )

    half = pl.ds(core * half_t, half_t)
    copies = around(
        n_ep, e,
        lambda k, p: remote(full.at[e, half], full.at[e, half], sems, 4, k, {"ep": p}),
    )
    own_gain = gain[:, pl.ds(pl.multiple_of(e * block, block), block)]
    own = (full[e].astype(F32).reshape(rows, block) * own_gain).astype(BF16)
    for i in range(2):
        loads[1 + i].wait()
        value = jnp.dot(own, (v_dgate, v_dup)[i][...], preferred_element_type=F32)
        dense_part[:, :, i * hidden : (i + 1) * hidden] = value.reshape(
            n_ep, seqs, hidden
        ).astype(BF16)
    dense_copies = around(
        n_ep, e,
        lambda k, p: remote(dense_part.at[p], dense_in.at[e], sems, 5, k, {"ep": p}),
    )
    passed = []
    for k in range(1, n_ep):
        copies[k - 1].wait_recv()
        origin = lax.rem(e + n_ep - k, n_ep)
        copy = remote(full.at[origin, half], full.at[origin, half], sems, 6, k, sibling)
        copy.start()
        passed.append(copy)
    for copy in copies:
        copy.wait_send()
    finish(passed)

    squares = jnp.zeros((rows, 1), F32)
    logit = jnp.zeros((rows, 1), F32)
    for j in range(n_ep):
        span = slice(j * block, (j + 1) * block)
        x = full[j].astype(F32).reshape(rows, block)
        squares = squares + jnp.sum(x * x, axis=1, keepdims=True)
        scaled = (x * gain[:, span]).astype(BF16).astype(F32)
        logit = logit + jnp.sum(scaled * branch[:, span].astype(F32), axis=1, keepdims=True)
    scale = lax.rsqrt(squares / width + EPS)
    branch_share = sigmoid(logit * scale)
    scale_ref[...] = jnp.broadcast_to(scale, scale_ref.shape)

    finish(dense_copies)
    total = dense_part[e].astype(F32)
    for k in range(1, n_ep):
        total = total + dense_in[lax.rem(e + k, n_ep)].astype(F32)
    total = total * scale_ref[pl.ds(pl.multiple_of(e * seqs, seqs), seqs), 0:1]
    gate = total[:, :hidden]
    dense_hid[e] = (gate * sigmoid(gate) * total[:, hidden:]).astype(BF16)
    copies = around(
        n_ep, e,
        lambda k, p: remote(dense_hid.at[e], dense_hid.at[e], sems, 7, k, {"ep": p}),
    )

    loads[3].wait()
    loads[4].wait()
    finish(share_copies)
    table = shares[...].reshape(rows, shares.shape[2])
    lane = lax.broadcasted_iota(jnp.int32, table.shape, 1)
    expert_hid, expert_share = [], []
    for l in range(local):
        gate = up = None
        for j in range(n_ep):
            span = slice(j * block, (j + 1) * block)
            x = (full[j].astype(F32).reshape(rows, block) * gain[:, span]).astype(BF16)
            g = jnp.dot(x, v_egate[l, span, :], preferred_element_type=F32)
            u = jnp.dot(x, v_eup[l, span, :], preferred_element_type=F32)
            gate = g if gate is None else gate + g
            up = u if up is None else up + u
        gate, up = gate * scale, up * scale
        expert_hid.append((gate * sigmoid(gate) * up).astype(BF16))
        expert_share.append(
            jnp.sum(jnp.where(lane == e * local + l, table, 0.0), axis=1, keepdims=True)
        )
    finish(copies)
    loads[5].wait()
    dense_out[...] = branch_share * jnp.dot(
        dense_hid[...].reshape(rows, hidden), v_ddown[...], preferred_element_type=F32
    )
    loads[6].wait()
    for j in range(n_ep):
        value = jnp.where(e == j, dense_out[...], 0.0)
        for l in range(local):
            value = value + expert_share[l] * jnp.dot(
                expert_hid[l],
                v_edown[l, :, j * block : (j + 1) * block],
                preferred_element_type=F32,
            )
        side, at = (j * block) // (width // 2), (j * block) % (width // 2)
        halves[side, :, :, at : at + block] = value.reshape(n_ep, seqs, block).astype(BF16)

    finish_pair = remote(halves.at[1 - core], half_in, sems, 8, 0, sibling)
    finish_pair.start()
    finish_pair.wait()
    summed[...] = (halves[core].astype(F32) + half_in[...].astype(F32)).astype(BF16)
    finish(
        around(
            n_ep, e, lambda k, p: remote(summed.at[p], summed_in.at[e], sems, 9, k, {"ep": p})
        )
    )
    total = summed[e].astype(F32)
    for k in range(1, n_ep):
        total = total + summed_in[lax.rem(e + k, n_ep)].astype(F32)
    for i in range(n_z):
        strips[i] = total[:, i * strip : (i + 1) * strip].astype(BF16)
    finish(
        around(
            n_z, z,
            lambda k, p: remote(
                strips.at[p], strips_in.at[z], sems, 10, k, {"tp": 2 * p + core}
            ),
        )
    )
    total = strips[z].astype(F32)
    for k in range(1, n_z):
        total = total + strips_in[lax.rem(z + k, n_z)].astype(F32)
    place = core * n_z + z
    per_block = block // strip
    held = full[
        lax.div(place, per_block),
        pl.ds(e * (seqs // chunk), seqs // chunk),
        :,
        pl.ds(pl.multiple_of(lax.rem(place, per_block) * strip, strip), strip),
    ]
    pieces[place] = (held.astype(F32).reshape(seqs, strip) + total).astype(BF16)
    finish(
        around(
            n_z, z,
            lambda k, p: remote(
                pieces.at[place], pieces.at[place], sems, 11, k, {"tp": 2 * p + core}
            ),
        )
    )
    side = pl.ds(core * n_z, n_z)
    copy = remote(pieces.at[side], pieces.at[side], sems, 12, 0, sibling)
    copy.start()
    copy.wait()
    for i in range(n_tp):
        out[:, i * strip : (i + 1) * strip] = pieces[i]


def on_device(
    n_ep, n_tp,
    tokens, state_matrix, state_norm, state_max, mixer_gain, w_query, w_key, w_value, w_outgate,
    w_ingate, w_forget, forget_bias, w_proj, ffn_gain, w_branch, routes, route_weight,
    expert_gate, expert_up, expert_down, dense_gate, dense_up, dense_down,
):
    seqs, width = tokens.shape
    heads, size = state_matrix.shape[1], state_matrix.shape[2]
    block, cols = w_query.shape
    heads_all = w_ingate.shape[1]
    vmem = pl.BlockSpec(memory_space=pltpu.VMEM)
    any_ = pl.BlockSpec(memory_space=pl.ANY)
    limit = 60 * 1024 * 1024

    proj, gates, spread = pl.pallas_call(
        functools.partial(project_kernel, n_ep, n_tp),
        out_shape=(
            jax.ShapeDtypeStruct((seqs, 4 * cols), F32),
            jax.ShapeDtypeStruct((seqs, 2 * heads), F32),
            jax.ShapeDtypeStruct((n_ep, seqs, block), BF16),
        ),
        in_specs=[vmem, vmem, any_, any_, any_, any_, any_, any_, vmem],
        out_specs=(vmem, vmem, vmem),
        scratch_shapes=[
            pltpu.VMEM((n_ep, seqs, block), BF16),
            pltpu.VMEM((4, block, cols), BF16),
            pltpu.VMEM((2, width, heads_all), BF16),
            pltpu.VMEM((n_ep, seqs, 4 * cols), BF16),
            pltpu.VMEM((n_ep, seqs, 4 * cols), BF16),
            pltpu.SemaphoreType.DMA((2, n_ep)),
            pltpu.SemaphoreType.DMA((2, n_ep)),
            pltpu.SemaphoreType.DMA((6,)),
        ],
        compiler_params=pltpu.CompilerParams(
            collective_id=0, has_side_effects=True, vmem_limit_bytes=limit
        ),
        name="project",
    )(
        tokens, mixer_gain.reshape(1, width), w_query, w_key, w_value, w_outgate,
        w_ingate, w_forget, forget_bias.reshape(1, heads_all),
    )

    group = 8
    mixed, new_matrix, new_norm, new_max = pl.pallas_call(
        cell_kernel,
        grid=(seqs // group,),
        out_shape=(
            jax.ShapeDtypeStruct((seqs, cols), F32),
            jax.ShapeDtypeStruct(state_matrix.shape, F32),
            jax.ShapeDtypeStruct(state_norm.shape, F32),
            jax.ShapeDtypeStruct(state_max.shape, F32),
        ),
        in_specs=[
            pl.BlockSpec((group, 4 * cols), lambda i: (i, 0)),
            pl.BlockSpec((group, 2 * heads), lambda i: (i, 0)),
            pl.BlockSpec((group, heads, size, size), lambda i: (i, 0, 0, 0)),
            pl.BlockSpec((group, heads, size), lambda i: (i, 0, 0)),
            pl.BlockSpec((group, heads), lambda i: (i, 0)),
        ],
        out_specs=(
            pl.BlockSpec((group, cols), lambda i: (i, 0)),
            pl.BlockSpec((group, heads, size, size), lambda i: (i, 0, 0, 0)),
            pl.BlockSpec((group, heads, size), lambda i: (i, 0, 0)),
            pl.BlockSpec((group, heads), lambda i: (i, 0)),
        ),
        name="cell",
    )(proj, gates, state_matrix, state_norm, state_max)

    rows = n_ep * seqs
    chunk = rows // n_tp
    hidden = dense_gate.shape[1]
    strip = width // n_tp
    lanes = -(-(n_ep * expert_gate.shape[0]) // 128) * 128
    phases, most = 13, max(n_ep, n_tp)
    layer_out = pl.pallas_call(
        functools.partial(ffn_kernel, n_ep, n_tp),
        out_shape=jax.ShapeDtypeStruct((seqs, width), BF16),
        in_specs=[vmem] * 6 + [any_] * 7,
        out_specs=vmem,
        scratch_shapes=[
            pltpu.VMEM(w.shape, BF16)
            for w in (w_proj, dense_gate, dense_up, expert_gate, expert_up, dense_down, expert_down)
        ]
        + [
            pltpu.VMEM((n_ep, seqs, cols), BF16),
            pltpu.VMEM((n_ep, seqs, lanes), F32),
            pltpu.VMEM((n_tp, chunk, block), BF16),
            pltpu.VMEM((n_tp, chunk, block), BF16),
            pltpu.VMEM((n_ep, n_tp, chunk, block), BF16),
            pltpu.VMEM((n_ep, seqs, 2 * hidden), BF16),
            pltpu.VMEM((n_ep, seqs, 2 * hidden), BF16),
            pltpu.VMEM((n_ep, seqs, hidden), BF16),
            pltpu.VMEM((rows, 128), F32),
            pltpu.VMEM((rows, block), F32),
            pltpu.VMEM((2, n_ep, seqs, width // 2), BF16),
            pltpu.VMEM((n_ep, seqs, width // 2), BF16),
            pltpu.VMEM((n_ep, seqs, width // 2), BF16),
            pltpu.VMEM((n_ep, seqs, width // 2), BF16),
            pltpu.VMEM((n_tp // 2, seqs, strip), BF16),
            pltpu.VMEM((n_tp // 2, seqs, strip), BF16),
            pltpu.VMEM((n_tp, seqs, strip), BF16),
            pltpu.SemaphoreType.DMA((phases, most)),
            pltpu.SemaphoreType.DMA((phases, most)),
            pltpu.SemaphoreType.DMA((7,)),
        ],
        compiler_params=pltpu.CompilerParams(
            collective_id=1, has_side_effects=True, vmem_limit_bytes=limit
        ),
        name="feedforward",
    )(
        mixed, spread.reshape(n_tp, chunk, block), ffn_gain.reshape(1, width),
        w_branch.reshape(1, width), routes, route_weight,
        w_proj, dense_gate, dense_up, expert_gate, expert_up, dense_down, expert_down,
    )
    return (layer_out, new_matrix, new_norm, new_max)


def solution(mesh):
    in_specs = (
        P("ep", None),
        P("ep", "tp", None, None),
        P("ep", "tp", None),
        P("ep", "tp"),
        P(),
        P("ep", "tp"),
        P("ep", "tp"),
        P("ep", "tp"),
        P("ep", "tp"),
        P(),
        P(),
        P(),
        P("tp", "ep"),
        P(),
        P(),
        P("ep", None),
        P("ep", None),
        P("ep", None, "tp"),
        P("ep", None, "tp"),
        P("ep", "tp", None),
        P("ep", "tp"),
        P("ep", "tp"),
        P("tp", "ep"),
    )
    out_specs = (P("ep", None), P("ep", "tp", None, None), P("ep", "tp", None), P("ep", "tp"))
    step = functools.partial(on_device, mesh.shape["ep"], mesh.shape["tp"])
    return jax.shard_map(step, mesh=mesh, in_specs=in_specs, out_specs=out_specs, check_vma=False)
```

```python
import functools

import jax
import jax.numpy as jnp
from jax import lax
from jax.experimental import pallas as pl
from jax.experimental.pallas import tpu as pltpu
from jax.sharding import PartitionSpec as P

EPS = 1e-06
F32 = jnp.float32
BF16 = jnp.bfloat16
MESH = pl.DeviceIdType.MESH


def remote(src, dst, sems, phase, k, peer):
    return pltpu.make_async_remote_copy(
        src_ref=src,
        dst_ref=dst,
        send_sem=sems[0].at[phase, k],
        recv_sem=sems[1].at[phase, k],
        device_id=peer,
        device_id_type=MESH,
    )


def around(n, me, make):
    copies = [make(k, lax.rem(me + k, n)) for k in range(1, n)]
    for copy in copies:
        copy.start()
    return copies


def finish(copies):
    for copy in copies:
        copy.wait()


def column(row):
    n = row.shape[1]
    down = lax.broadcasted_iota(jnp.int32, (n, n), 0)
    along = lax.broadcasted_iota(jnp.int32, (n, n), 1)
    spread_row = jnp.broadcast_to(row, (n, n))
    return jnp.sum(jnp.where(down == along, spread_row, 0.0), axis=1, keepdims=True)


def project_kernel(
    n_ep, n_tp,
    tokens, gain, w_q, w_k, w_v, w_o, w_in, w_fg, bias, top,
    proj, gates, new_top, spread,
    arrived, weights, gate_w, outgoing, incoming, send_sem, recv_sem, load_sem,
):
    e, t = lax.axis_index("ep"), lax.axis_index("tp")
    seqs, width = tokens.shape
    block = width // n_ep
    cols = w_q.shape[1]
    heads_all = bias.shape[1]
    heads = heads_all // n_tp
    sems = (send_sem, recv_sem)
    barrier = pltpu.get_barrier_semaphore()
    for k in range(1, n_ep):
        pl.semaphore_signal(
            barrier, inc=1, device_id={"ep": lax.rem(e + k, n_ep)}, device_id_type=MESH
        )
    loads = [
        pltpu.make_async_copy(src, dst, load_sem.at[i])
        for i, (src, dst) in enumerate(
            [(w_in, gate_w.at[0]), (w_fg, gate_w.at[1])]
            + [(w, weights.at[j]) for j, w in enumerate((w_q, w_k, w_v, w_o))]
        )
    ]
    for load in loads:
        load.start()
    pl.semaphore_wait(barrier, n_ep - 1)

    def columns(index):
        return pl.ds(pl.multiple_of(index * block, block), block)

    copies = around(
        n_ep, e,
        lambda k, p: remote(tokens.at[:, columns(p)], arrived.at[e], sems, 0, k, {"ep": p}),
    )
    wide = tokens[...].astype(F32)
    scale = lax.rsqrt(jnp.mean(wide * wide, axis=1, keepdims=True) + EPS)
    normed = (wide * scale * gain[...]).astype(BF16)
    loads[0].wait()
    loads[1].wait()
    contract = (((1,), (1,)), ((), ()))
    gate_in = lax.dot_general(gate_w[0], normed, contract, preferred_element_type=F32)
    gate_fg = lax.dot_general(gate_w[1], normed, contract, preferred_element_type=F32)
    down = lax.broadcasted_iota(jnp.int32, gate_in.shape, 0)
    along = lax.broadcasted_iota(jnp.int32, bias.shape, 1)
    for h in range(heads):
        head = t * heads + h
        shift = jnp.sum(jnp.where(along == head, bias[...], 0.0), axis=1, keepdims=True)
        entry = jnp.sum(jnp.where(down == head, gate_in, 0.0), axis=0, keepdims=True)
        forget = jnp.sum(jnp.where(down == head, gate_fg, 0.0), axis=0, keepdims=True) + shift
        log_keep = jnp.minimum(forget, 0.0) - jnp.log1p(jnp.exp(-jnp.abs(forget)))
        kept = log_keep + top[h : h + 1, :]
        highest = jnp.maximum(kept, entry)
        new_top[h : h + 1, :] = highest
        gates[:, h : h + 1] = column(jnp.exp(kept - highest))
        gates[:, heads + h : heads + h + 1] = column(jnp.exp(entry - highest))
    spread[e] = tokens[:, columns(e)]
    finish(copies)
    for k in range(1, n_ep):
        p = lax.rem(e + k, n_ep)
        spread[p] = arrived[p]
    scaled = spread[...].astype(F32).reshape(n_ep * seqs, block) * gain[:, columns(e)]
    scaled = scaled.astype(BF16)
    for j in range(4):
        loads[2 + j].wait()
        part = jnp.dot(scaled, weights[j], preferred_element_type=F32)
        outgoing[:, :, j * cols : (j + 1) * cols] = part.reshape(n_ep, seqs, cols).astype(BF16)
    finish(
        around(
            n_ep, e,
            lambda k, p: remote(outgoing.at[p], incoming.at[e], sems, 1, k, {"ep": p}),
        )
    )
    total = outgoing[e].astype(F32)
    for k in range(1, n_ep):
        total = total + incoming[lax.rem(e + k, n_ep)].astype(F32)
    proj[...] = total * scale


def cell_kernel(proj, gates, matrix, norm, top, mixed, new_matrix, new_norm, new_top):
    new_top[...] = top[...]
    rows, heads, size, _ = matrix.shape
    keep = gates[:, :heads]
    write = gates[:, heads:]
    width = heads * size
    for h in range(heads):
        at = h * size
        q = proj[:, at : at + size]
        key = proj[:, width + at : width + at + size] * (size ** (-0.5))
        val = proj[:, 2 * width + at : 2 * width + at + size]
        gate = proj[:, 3 * width + at : 3 * width + at + size]
        keep_h = keep[:, h : h + 1]
        added = write[:, h : h + 1] * key
        normal = keep_h * norm[:, h, :] + added
        new_norm[:, h, :] = normal
        denom = jnp.maximum(jnp.abs(jnp.sum(q * normal, axis=1, keepdims=True)), 1.0)
        q_t = q.T
        added_t = added.T
        numer = []
        for b in range(rows):
            fresh = keep_h[b : b + 1] * matrix[b, h] + added_t[:, b : b + 1] * val[b : b + 1]
            new_matrix[b, h] = fresh
            numer.append(jnp.sum(q_t[:, b : b + 1] * fresh, axis=0, keepdims=True))
        cell = jnp.concatenate(numer, axis=0) / denom
        mixed[:, at : at + size] = cell / (1.0 + jnp.exp(-gate))


def sigmoid(x):
    return 1.0 / (1.0 + jnp.exp(-x))


def ffn_kernel(
    n_ep, n_tp,
    mixed, spread, gain, branch, routes, route_weight,
    w_proj, d_gate, d_up, e_gate, e_up, d_down, e_down,
    out,
    v_proj, v_dgate, v_dup, v_egate, v_eup, v_ddown, v_edown,
    heads_all, shares, part, part_in, part_sum, part_z, full, dense_part, dense_in, dense_hid,
    scale_ref, halves, half_in, summed, summed_in, strips, strips_in, pieces,
    send_sem, recv_sem, ep_send, ep_recv, fw_send, fw_recv, rs_send, rs_recv, load_sem,
):
    e, t = lax.axis_index("ep"), lax.axis_index("tp")
    core = lax.rem(t, 2)
    z = lax.div(t, 2)
    n_z = n_tp // 2
    seqs = mixed.shape[0]
    rows = n_ep * seqs
    chunk, block = spread.shape[1], spread.shape[2]
    width = n_ep * block
    hidden = d_gate.shape[1]
    local = e_gate.shape[0]
    sems = (send_sem, recv_sem)
    sibling = {"tp": t + 1 - 2 * core}
    strip = width // n_tp

    barrier = pltpu.get_barrier_semaphore()
    for k in range(1, n_ep):
        pl.semaphore_signal(
            barrier, inc=1, device_id={"ep": lax.rem(e + k, n_ep)}, device_id_type=MESH
        )
    for k in range(1, n_z):
        pl.semaphore_signal(
            barrier, inc=1, device_id={"tp": lax.rem(t + 2 * k, n_tp)}, device_id_type=MESH
        )
    pl.semaphore_signal(barrier, inc=1, device_id=sibling, device_id_type=MESH)
    loads = [
        pltpu.make_async_copy(src, dst, load_sem.at[i])
        for i, (src, dst) in enumerate(
            [(w_proj, v_proj), (d_gate, v_dgate), (d_up, v_dup), (e_gate, v_egate),
             (e_up, v_eup), (d_down, v_ddown), (e_down, v_edown)]
        )
    ]
    for load in loads:
        load.start()

    heads_all[e] = mixed[...].astype(BF16)
    weight = route_weight[...]
    share = weight / jnp.sum(weight, axis=0, keepdims=True)
    named = routes[...].astype(F32)
    lane = lax.broadcasted_iota(jnp.int32, (seqs, shares.shape[2]), 1)
    table = jnp.zeros((seqs, shares.shape[2]), F32)
    for k in range(routes.shape[0]):
        chosen = lane.astype(F32) == column(named[k : k + 1])
        table = table + jnp.where(chosen, column(share[k : k + 1]), 0.0)
    shares[e] = table
    pl.semaphore_wait(barrier, n_ep + n_z - 1)

    copies = around(
        n_ep, e,
        lambda k, p: remote(heads_all.at[e], heads_all.at[e], sems, 0, k, {"ep": p}),
    )
    share_copies = around(
        n_ep, e, lambda k, p: remote(shares.at[e], shares.at[e], sems, 1, k, {"ep": p})
    )
    loads[0].wait()
    finish(copies)
    cols = heads_all.shape[2]
    mixer = jnp.dot(
        heads_all[...].reshape(rows, cols), v_proj[...], preferred_element_type=F32
    )
    part[...] = mixer.reshape(2, n_z, chunk, block).astype(BF16)
    copy = remote(part.at[1 - core], part_in, sems, 2, 0, sibling)
    copy.start()
    copy.wait()
    part_sum[...] = (part[core].astype(F32) + part_in[...].astype(F32)).astype(BF16)
    finish(
        around(
            n_z, z,
            lambda k, p: remote(
                part_sum.at[p], part_z.at[z], sems, 3, k, {"tp": 2 * p + core}
            ),
        )
    )
    total = part_sum[z].astype(F32)
    for k in range(1, n_z):
        total = total + part_z[lax.rem(z + k, n_z)].astype(F32)
    place = core * n_z + z
    full[e, place] = (spread[place].astype(F32) + total).astype(BF16)

    def same(a, b, sem_pair, i, k, peer):
        return remote(full.at[a, b], full.at[a, b], sem_pair, i, k, peer)

    z_copies = around(
        n_z, z, lambda k, p: same(e, place, sems, 4, k, {"tp": 2 * p + core})
    )
    ep_sems, fw_sems = (ep_send, ep_recv), (fw_send, fw_recv)
    ep_copies, passed = [], []
    for i in range(n_z):
        spot = core * n_z + lax.rem(z + n_z - i, n_z)
        if i > 0:
            z_copies[i - 1].wait_recv()
        passed.append(same(e, spot, fw_sems, i, 0, sibling))
        passed[-1].start()
        ep_copies.append(
            around(n_ep, e, lambda k, p: same(e, spot, ep_sems, i, k, {"ep": p}))
        )
    finish(passed)
    own_gain = gain[:, pl.ds(pl.multiple_of(e * block, block), block)]
    own = (full[e].astype(F32).reshape(rows, block) * own_gain).astype(BF16)
    for i in range(2):
        loads[1 + i].wait()
        value = jnp.dot(own, (v_dgate, v_dup)[i][...], preferred_element_type=F32)
        dense_part[:, :, i * hidden : (i + 1) * hidden] = value.reshape(
            n_ep, seqs, hidden
        ).astype(BF16)
    dense_copies = around(
        n_ep, e,
        lambda k, p: remote(dense_part.at[p], dense_in.at[e], sems, 6, k, {"ep": p}),
    )
    passed = []
    for i in range(n_z):
        spot = core * n_z + lax.rem(z + n_z - i, n_z)
        for k in range(1, n_ep):
            ep_copies[i][k - 1].wait_recv()
            passed.append(same(lax.rem(e + n_ep - k, n_ep), spot, fw_sems, i, k, sibling))
            passed[-1].start()
    for copy in z_copies:
        copy.wait_send()
    for group in ep_copies:
        for copy in group:
            copy.wait_send()
    finish(passed)

    squares = jnp.zeros((rows, 1), F32)
    logit = jnp.zeros((rows, 1), F32)
    for j in range(n_ep):
        span = slice(j * block, (j + 1) * block)
        x = full[j].astype(F32).reshape(rows, block)
        squares = squares + jnp.sum(x * x, axis=1, keepdims=True)
        scaled = (x * gain[:, span]).astype(BF16).astype(F32)
        logit = logit + jnp.sum(scaled * branch[:, span].astype(F32), axis=1, keepdims=True)
    scale = lax.rsqrt(squares / width + EPS)
    branch_share = sigmoid(logit * scale)
    scale_ref[...] = jnp.broadcast_to(scale, scale_ref.shape)

    loads[3].wait()
    loads[4].wait()
    finish(share_copies)
    table = shares[...].reshape(rows, shares.shape[2])
    lane = lax.broadcasted_iota(jnp.int32, table.shape, 1)
    expert_hid, expert_share = [], []
    for l in range(local):
        gate = up = None
        for j in range(n_ep):
            span = slice(j * block, (j + 1) * block)
            x = (full[j].astype(F32).reshape(rows, block) * gain[:, span]).astype(BF16)
            g = jnp.dot(x, v_egate[l, span, :], preferred_element_type=F32)
            u = jnp.dot(x, v_eup[l, span, :], preferred_element_type=F32)
            gate = g if gate is None else gate + g
            up = u if up is None else up + u
        gate, up = gate * scale, up * scale
        expert_hid.append((gate * sigmoid(gate) * up).astype(BF16))
        expert_share.append(
            jnp.sum(jnp.where(lane == e * local + l, table, 0.0), axis=1, keepdims=True)
        )
    finish(dense_copies)
    total = dense_part[e].astype(F32)
    for k in range(1, n_ep):
        total = total + dense_in[lax.rem(e + k, n_ep)].astype(F32)
    total = total * scale_ref[pl.ds(pl.multiple_of(e * seqs, seqs), seqs), 0:1]
    gate = total[:, :hidden]
    dense_hid[e] = (gate * sigmoid(gate) * total[:, hidden:]).astype(BF16)
    copies = around(
        n_ep, e,
        lambda k, p: remote(dense_hid.at[e], dense_hid.at[e], sems, 7, k, {"ep": p}),
    )

    loads[6].wait()
    for j in range(n_ep):
        value = None
        for l in range(local):
            term = expert_share[l] * jnp.dot(
                expert_hid[l],
                v_edown[l, :, j * block : (j + 1) * block],
                preferred_element_type=F32,
            )
            value = term if value is None else value + term
        side, at = (j * block) // (width // 2), (j * block) % (width // 2)
        halves[side, :, :, at : at + block] = value.reshape(n_ep, seqs, block).astype(BF16)
    finish(copies)
    loads[5].wait()
    dense_out = branch_share * jnp.dot(
        dense_hid[...].reshape(rows, hidden), v_ddown[...], preferred_element_type=F32
    )
    per_half = n_ep // 2
    side = lax.div(e, per_half)
    at = pl.ds(pl.multiple_of(lax.rem(e, per_half) * block, block), block)
    halves[side, :, :, at] = (
        halves[side, :, :, at].astype(F32) + dense_out.reshape(n_ep, seqs, block)
    ).astype(BF16)

    finish_pair = remote(halves.at[1 - core], half_in, sems, 5, 0, sibling)
    finish_pair.start()
    finish_pair.wait()
    for i in range(n_z):
        cut = slice(i * strip, (i + 1) * strip)
        summed[i] = (
            halves[core, :, :, cut].astype(F32) + half_in[:, :, cut].astype(F32)
        ).astype(BF16)
    rs_sems = (rs_send, rs_recv)
    order = [lax.rem(z + i, n_z) for i in range(1, n_z + 1)]
    scatter = [
        around(
            n_ep, e,
            lambda k, p: remote(
                summed.at[q, p], summed_in.at[q, e], rs_sems, i, k, {"ep": p}
            ),
        )
        for i, q in enumerate(order)
    ]
    z_copies = []
    for i, q in enumerate(order):
        finish(scatter[i])
        total = summed[q, e].astype(F32)
        for k in range(1, n_ep):
            total = total + summed_in[q, lax.rem(e + k, n_ep)].astype(F32)
        if i < n_z - 1:
            strips[q] = total.astype(BF16)
            z_copies.append(
                remote(strips.at[q], strips_in.at[z], sems, 8, i + 1, {"tp": 2 * q + core})
            )
            z_copies[-1].start()
    finish(z_copies)
    for k in range(1, n_z):
        total = total + strips_in[lax.rem(z + k, n_z)].astype(F32)
    per_block = block // strip
    held = full[
        lax.div(place, per_block),
        pl.ds(e * (seqs // chunk), seqs // chunk),
        :,
        pl.ds(pl.multiple_of(lax.rem(place, per_block) * strip, strip), strip),
    ]
    pieces[place] = (held.astype(F32).reshape(seqs, strip) + total).astype(BF16)
    z_copies = around(
        n_z, z,
        lambda k, p: remote(
            pieces.at[place], pieces.at[place], sems, 9, k, {"tp": 2 * p + core}
        ),
    )
    passed = []
    for i in range(n_z):
        spot = core * n_z + lax.rem(z + n_z - i, n_z)
        if i > 0:
            z_copies[i - 1].wait_recv()
        passed.append(remote(pieces.at[spot], pieces.at[spot], sems, 10, i, sibling))
        passed[-1].start()
    for copy in z_copies:
        copy.wait_send()
    finish(passed)
    for i in range(n_tp):
        out[:, i * strip : (i + 1) * strip] = pieces[i]


def on_device(
    n_ep, n_tp,
    tokens, state_matrix, state_norm, state_max, mixer_gain, w_query, w_key, w_value, w_outgate,
    w_ingate, w_forget, forget_bias, w_proj, ffn_gain, w_branch, routes, route_weight,
    expert_gate, expert_up, expert_down, dense_gate, dense_up, dense_down,
):
    seqs, width = tokens.shape
    heads, size = state_matrix.shape[1], state_matrix.shape[2]
    block, cols = w_query.shape
    heads_all = w_ingate.shape[1]
    vmem = pl.BlockSpec(memory_space=pltpu.VMEM)
    any_ = pl.BlockSpec(memory_space=pl.ANY)
    limit = 60 * 1024 * 1024

    proj, gates, top, spread = pl.pallas_call(
        functools.partial(project_kernel, n_ep, n_tp),
        out_shape=(
            jax.ShapeDtypeStruct((seqs, 4 * cols), F32),
            jax.ShapeDtypeStruct((seqs, 2 * heads), F32),
            jax.ShapeDtypeStruct((heads, seqs), F32),
            jax.ShapeDtypeStruct((n_ep, seqs, block), BF16),
        ),
        in_specs=[vmem, vmem, any_, any_, any_, any_, any_, any_, vmem, vmem],
        out_specs=(vmem, vmem, vmem, vmem),
        scratch_shapes=[
            pltpu.VMEM((n_ep, seqs, block), BF16),
            pltpu.VMEM((4, block, cols), BF16),
            pltpu.VMEM((2, heads_all, width), BF16),
            pltpu.VMEM((n_ep, seqs, 4 * cols), BF16),
            pltpu.VMEM((n_ep, seqs, 4 * cols), BF16),
            pltpu.SemaphoreType.DMA((2, n_ep)),
            pltpu.SemaphoreType.DMA((2, n_ep)),
            pltpu.SemaphoreType.DMA((6,)),
        ],
        compiler_params=pltpu.CompilerParams(
            collective_id=0, has_side_effects=True, vmem_limit_bytes=limit
        ),
        name="project",
    )(
        tokens, mixer_gain.reshape(1, width), w_query, w_key, w_value, w_outgate,
        w_ingate.T, w_forget.T, forget_bias.reshape(1, heads_all), state_max.T,
    )

    group = 8
    mixed, new_matrix, new_norm, new_max = pl.pallas_call(
        cell_kernel,
        grid=(seqs // group,),
        out_shape=(
            jax.ShapeDtypeStruct((seqs, cols), F32),
            jax.ShapeDtypeStruct(state_matrix.shape, F32),
            jax.ShapeDtypeStruct(state_norm.shape, F32),
            jax.ShapeDtypeStruct((heads, seqs), F32),
        ),
        in_specs=[
            pl.BlockSpec((group, 4 * cols), lambda i: (i, 0)),
            pl.BlockSpec((group, 2 * heads), lambda i: (i, 0)),
            pl.BlockSpec((group, heads, size, size), lambda i: (i, 0, 0, 0)),
            pl.BlockSpec((group, heads, size), lambda i: (i, 0, 0)),
            pl.BlockSpec((heads, seqs), lambda i: (0, 0)),
        ],
        out_specs=(
            pl.BlockSpec((group, cols), lambda i: (i, 0)),
            pl.BlockSpec((group, heads, size, size), lambda i: (i, 0, 0, 0)),
            pl.BlockSpec((group, heads, size), lambda i: (i, 0, 0)),
            pl.BlockSpec((heads, seqs), lambda i: (0, 0)),
        ),
        name="cell",
    )(proj, gates, state_matrix, state_norm, top)

    rows = n_ep * seqs
    chunk = rows // n_tp
    hidden = dense_gate.shape[1]
    strip = width // n_tp
    lanes = -(-(n_ep * expert_gate.shape[0]) // 128) * 128
    phases, most = 11, max(n_ep, n_tp)
    layer_out = pl.pallas_call(
        functools.partial(ffn_kernel, n_ep, n_tp),
        out_shape=jax.ShapeDtypeStruct((seqs, width), BF16),
        in_specs=[vmem] * 6 + [any_] * 7,
        out_specs=vmem,
        scratch_shapes=[
            pltpu.VMEM(w.shape, BF16)
            for w in (w_proj, dense_gate, dense_up, expert_gate, expert_up, dense_down, expert_down)
        ]
        + [
            pltpu.VMEM((n_ep, seqs, cols), BF16),
            pltpu.VMEM((n_ep, seqs, lanes), F32),
            pltpu.VMEM((2, n_tp // 2, chunk, block), BF16),
            pltpu.VMEM((n_tp // 2, chunk, block), BF16),
            pltpu.VMEM((n_tp // 2, chunk, block), BF16),
            pltpu.VMEM((n_tp // 2, chunk, block), BF16),
            pltpu.VMEM((n_ep, n_tp, chunk, block), BF16),
            pltpu.VMEM((n_ep, seqs, 2 * hidden), BF16),
            pltpu.VMEM((n_ep, seqs, 2 * hidden), BF16),
            pltpu.VMEM((n_ep, seqs, hidden), BF16),
            pltpu.VMEM((rows, 128), F32),
            pltpu.VMEM((2, n_ep, seqs, width // 2), BF16),
            pltpu.VMEM((n_ep, seqs, width // 2), BF16),
            pltpu.VMEM((n_tp // 2, n_ep, seqs, strip), BF16),
            pltpu.VMEM((n_tp // 2, n_ep, seqs, strip), BF16),
            pltpu.VMEM((n_tp // 2, seqs, strip), BF16),
            pltpu.VMEM((n_tp // 2, seqs, strip), BF16),
            pltpu.VMEM((n_tp, seqs, strip), BF16),
            pltpu.SemaphoreType.DMA((phases, most)),
            pltpu.SemaphoreType.DMA((phases, most)),
        ]
        + [pltpu.SemaphoreType.DMA((n_tp // 2, n_ep))] * 6
        + [
            pltpu.SemaphoreType.DMA((7,)),
        ],
        compiler_params=pltpu.CompilerParams(
            collective_id=1, has_side_effects=True, vmem_limit_bytes=limit
        ),
        name="feedforward",
    )(
        mixed, spread.reshape(n_tp, chunk, block), ffn_gain.reshape(1, width),
        w_branch.reshape(1, width), routes.T, route_weight.T,
        w_proj, dense_gate, dense_up, expert_gate, expert_up, dense_down, expert_down,
    )
    return (layer_out, new_matrix, new_norm, new_max.T)


def solution(mesh):
    in_specs = (
        P("ep", None),
        P("ep", "tp", None, None),
        P("ep", "tp", None),
        P("ep", "tp"),
        P(),
        P("ep", "tp"),
        P("ep", "tp"),
        P("ep", "tp"),
        P("ep", "tp"),
        P(),
        P(),
        P(),
        P("tp", "ep"),
        P(),
        P(),
        P("ep", None),
        P("ep", None),
        P("ep", None, "tp"),
        P("ep", None, "tp"),
        P("ep", "tp", None),
        P("ep", "tp"),
        P("ep", "tp"),
        P("tp", "ep"),
    )
    out_specs = (P("ep", None), P("ep", "tp", None, None), P("ep", "tp", None), P("ep", "tp"))
    step = functools.partial(on_device, mesh.shape["ep"], mesh.shape["tp"])
    return jax.shard_map(step, mesh=mesh, in_specs=in_specs, out_specs=out_specs, check_vma=False)
```
